32 devices in a mesh: sp: 8 (over z, y), tp: 4 (over x, core).
Axes of the slice: x: 2, y: 2, z: 4, core: 2. Of those that a mesh axis runs over, the one named last changes fastest.
Arguments:
- hidden: bfloat16 [2048, 2048], P('sp'), may hold values from -6 to 6
- cotangent: bfloat16 [2048, 2048], P('sp'), may hold values from -6 to 6
- retained: bfloat16 [2048, 2048], P('sp', 'tp'), may hold values from -6 to 6
- queries: bfloat16 [2048, 1024], P('sp', 'tp'), may hold values from -1.5 to 1.5
- key_rows: bfloat16 [2048, 1024], P('sp', 'tp'), may hold values from -1.5 to 1.5
- value_rows: bfloat16 [2048, 2048], P('sp', 'tp'), may hold values from -0.25 to 0.25
- routes: int32 [2048, 2], P('sp'), may hold values from 0 to 7, all different within a row; in each aligned block of 256 rows (0 to 255, 256 to 511, ...) at most 96 rows name the same one
- route_weight: float32 [2048, 2], P('sp'), may hold values from 0.2 to 1.5
- gate_weight: bfloat16 [8, 2048, 1024], P('sp', None, 'tp'), may hold values from -0.125 to 0.125
- up_weight: bfloat16 [8, 2048, 1024], P('sp', None, 'tp'), may hold values from -0.125 to 0.125
- down_weight: bfloat16 [8, 1024, 2048], P('sp', 'tp'), may hold values from -0.1875 to 0.1875
- out_weight: bfloat16 [2048, 2048], P(None, 'tp'), may hold values from -0.125 to 0.125
Outputs:
- gate_grad: float32 [8, 2048, 1024], P('sp', None, 'tp')
- up_grad: float32 [8, 2048, 1024], P('sp', None, 'tp')
- down_grad: float32 [8, 1024, 2048], P('sp', 'tp')
- proj_grad: float32 [2048, 2048], P('sp', 'tp')
- query_gradient: float32 [2048, 1024], P('sp', 'tp')
- key_gradient: float32 [2048, 1024], P('sp', 'tp')
- value_gradient: float32 [2048, 2048], P('sp', 'tp')
The draws below stay inside these ranges and needn't reach their ends.
Inputs may be any that keep to these rules, and one draw needn't show every extreme that they name: `routes`: each row names 2 different experts; among the 256 rows of one index of sp no expert is named more than 96 times, a bound that some block reaches.
All inputs are finite; a program needn't handle non-finite values.
Results may differ from the reference program's by a relative error of at most 0.013.
Values may be sent and summed in bfloat16 or wider, within the bound.
A program may use at most 128 MiB of HBM per device.

```python
import math
import jax
import jax.numpy as jnp
import numpy as np
from jax import lax

D = 2048
H = 4
DK = 256
DV = 512
FF = 1024
TOP = 2
TOK_DEV = 256
TOKENS = 2048
EXPERTS = 8
CAP = 96
VW = 2048
N_SP = 8
N_TP = 4


def with_spikes(array, own_key, source, target, blocks, factor):
    owner, partner = [(jnp.arange(array.shape[position]) // (array.shape[position] // blocks)).reshape([-1 if axis == position else 1 for axis in range(array.ndim)]) for position in (source, target)]
    chosen = jax.random.permutation(own_key, blocks)[partner]
    strong = (owner == chosen) | (owner == (partner + blocks // 2) % blocks)
    return jnp.where(strong, factor * array, array)


def block_scale(own_key, shape, cuts, smallest, largest):
    level = 1.0
    for position, blocks in cuts:
        heights = jax.random.uniform(jax.random.fold_in(jax.random.fold_in(own_key, 6), position), (blocks,), jnp.float32, smallest / len(cuts), largest / len(cuts))
        level = level * jnp.repeat(jnp.exp(heights), shape[position] // blocks).reshape((-1,) + (1,) * (len(shape) - 1 - position))
    return level


def assign_block(key, own, number, rows, number_of, top, most, skew):
    sequence = jax.random.permutation(key, number_of)
    heavy_load, ordinary = portions_of(number_of, rows * top, most, skew, True), portions_of(number_of, rows * top, most, skew, False)
    places = jnp.arange(number_of)

    def named(tallies, offset_by):
        used = int((tallies > 0).sum())
        fixed = max(1, used // 4)
        passed = fixed + (places - fixed + offset_by * (used - fixed)) % max(1, number_of - fixed)
        return jnp.zeros((number_of,), jnp.int32).at[sequence[jnp.where(places < fixed, places, passed)]].set(jnp.asarray(tallies, jnp.int32))

    tallies = jnp.where(number % 4 == 0, named(heavy_load, number // 4), named(ordinary, number - number // 4 - 1))
    mixed = jax.random.permutation(jax.random.fold_in(own, 3), number_of)
    source_of, receiver = mixed[0:number_of // 2 * 2:2], mixed[1:number_of // 2 * 2:2]
    slack = jnp.minimum(tallies[source_of] - 1, most - tallies[receiver]) // 2
    slack = jnp.where((source_of == sequence[0]) | (receiver == sequence[0]) | (tallies[receiver] == 0), 0, jnp.maximum(slack, 0))
    passed = jax.random.randint(jax.random.fold_in(own, 4), (number_of // 2,), 0, 1 << 20) % (slack + 1)
    tallies = tallies.at[source_of].add(-passed).at[receiver].add(passed)
    members = jnp.searchsorted(jnp.cumsum(tallies), jnp.arange(rows * top), side="right").astype(jnp.int32)
    listing = members.reshape(top, rows).T
    listing = listing[jax.random.permutation(jax.random.fold_in(own, 1), rows)]
    offset_by = jax.random.randint(jax.random.fold_in(own, 2), (rows, 1), 0, top)
    return jnp.take_along_axis(listing, (jnp.arange(top)[None, :] + offset_by) % top, axis=1)


def portions_of(number_of, total, reach, lean, full):
    weights = [(1 << 20) // math.isqrt(rank ** lean) + 1 for rank in range(1, number_of + 1)]
    largest = reach if full else min(reach, max(-(-total // number_of), total * weights[0] // sum(weights)))
    least = 1 if total - largest >= number_of - 1 else 0
    counts, surplus = [largest] + [least] * (number_of - 1), total - largest - least * (number_of - 1)
    while surplus > 0:
        movable = [i for i in range(1, number_of) if counts[i] < largest] or [i for i in range(1, number_of) if counts[i] < reach]
        mass, left = sum([weights[i] for i in movable]), surplus
        for i in movable:
            addition = min(reach - counts[i], max(1, left * weights[i] // mass), surplus)
            counts[i] = counts[i] + addition
            surplus = surplus - addition
    return np.array(counts)


def centred(rng, dims, scale, limit, cuts=(), kind=jnp.bfloat16):
    entries = scale * jax.random.normal(rng, dims, jnp.float32)
    if cuts:
        entries = entries * block_scale(rng, dims, cuts, -0.22, 0.18)
    return jnp.clip(entries, -limit, limit).astype(kind)


def bell_draw_with(key, dims, width, limit, cuts, heavy, kind=jnp.bfloat16):
    entries = width * jax.random.normal(key, dims, jnp.float32)
    if cuts:
        entries = entries * block_scale(key, dims, cuts, -0.22, 0.18)
    return jnp.clip(with_spikes(entries, jax.random.fold_in(key, 3), *heavy), -limit, limit).astype(kind)


def setup_inputs(seed: int = 0) -> dict:
    keys = jax.random.split(jax.random.key(seed), 13)
    hidden = centred(keys[0], (TOKENS, D), 1.0, 6.0, ((0, 8),))
    cotangent = bell_draw_with(keys[1], (TOKENS, D), 1.0, 6.0, ((0, 8),), (0, 1, 8, 2.0))
    retained = centred(keys[2], (TOKENS, VW), 1.0, 6.0, ((0, 8), (1, 4)))
    queries = centred(keys[3], (TOKENS, H * DK), 0.25, 1.5, ((0, 8), (1, 4)))
    key_rows = centred(keys[4], (TOKENS, H * DK), 0.25, 1.5, ((0, 8), (1, 4)))
    value_rows = centred(keys[5], (TOKENS, VW), DV ** -0.5, 0.25, ((0, 8), (1, 4)))
    routes_keys = jax.random.split(jax.random.fold_in(keys[6], 1), TOKENS // TOK_DEV)
    routes_turns = jax.random.permutation(jax.random.fold_in(keys[6], 3), TOKENS // TOK_DEV)
    routes = jax.vmap(lambda own, number: assign_block(jax.random.fold_in(keys[6], 2), own, number, TOK_DEV, EXPERTS, TOP, CAP, 2))(routes_keys, routes_turns).reshape((TOKENS, TOP))
    route_weight = jnp.clip(0.2 + 1.3 * jax.random.uniform(keys[7], (TOKENS, TOP), jnp.float32) ** block_scale(keys[7], (TOKENS, TOP), ((0, 8),), -0.2, 0.2), 0.2, 1.5)
    gate_weight = centred(keys[8], (EXPERTS, D, FF), D ** -0.5, 0.125, ((0, 8), (2, 4)))
    up_weight = centred(keys[9], (EXPERTS, D, FF), D ** -0.5, 0.125, ((0, 8), (2, 4)))
    down_weight = centred(keys[10], (EXPERTS, FF, D), FF ** -0.5, 0.1875, ((0, 8), (1, 4)))
    out_weight = centred(keys[11], (D, VW), VW ** -0.5, 0.125, ((1, 4),))
    return dict(hidden=hidden, cotangent=cotangent, retained=retained, queries=queries, key_rows=key_rows, value_rows=value_rows, routes=routes, route_weight=route_weight, gate_weight=gate_weight, up_weight=up_weight, down_weight=down_weight, out_weight=out_weight)


def expert_backward(inputs, upstream, gate_matrix, up_matrix, down_matrix):
    gate_pre = jnp.dot(inputs, gate_matrix, preferred_element_type=jnp.float32)
    up_pre = jnp.dot(inputs, up_matrix, preferred_element_type=jnp.float32)
    sigma = jax.nn.sigmoid(gate_pre)
    active = gate_pre * sigma
    product = (active * up_pre).astype(jnp.bfloat16)
    down_part = jnp.dot(product.T, upstream, preferred_element_type=jnp.float32)
    unit_grad = jnp.dot(upstream, down_matrix.T, preferred_element_type=jnp.float32)
    gate_term = (unit_grad * up_pre * sigma * (1.0 + gate_pre * (1.0 - sigma))).astype(jnp.bfloat16)
    up_term = (unit_grad * active).astype(jnp.bfloat16)
    gate_part = jnp.dot(inputs.T, gate_term, preferred_element_type=jnp.float32)
    up_part = jnp.dot(inputs.T, up_term, preferred_element_type=jnp.float32)
    rows = gate_term.shape[0]
    group = FF // N_TP
    gate_split = gate_term.astype(jnp.float32).reshape(rows, N_TP, group)
    up_split = up_term.astype(jnp.float32).reshape(rows, N_TP, group)
    gate_cols = gate_matrix.astype(jnp.float32).reshape(D, N_TP, group)
    up_cols = up_matrix.astype(jnp.float32).reshape(D, N_TP, group)
    row_part = jnp.einsum('rnf,dnf->nrd', gate_split, gate_cols) + jnp.einsum('rnf,dnf->nrd', up_split, up_cols)
    return (gate_part, up_part, down_part, row_part.astype(jnp.bfloat16))

def slot_targets(routes):
    flat = routes.reshape(N_SP, TOK_DEV * TOP)
    onehot = (flat[:, :, None] == jnp.arange(EXPERTS, dtype=jnp.int32)[None, None, :]).astype(jnp.int32)
    rank = lax.optimization_barrier(jnp.sum(jnp.cumsum(onehot, axis=1) * onehot, axis=2)) - 1
    block = jnp.arange(N_SP, dtype=jnp.int32)[:, None]
    return (flat * (N_SP * CAP) + block * CAP + rank).reshape(-1).astype(jnp.int32)

def head_rates(head_ids, total_tokens):
    ids = head_ids.astype(jnp.float32)
    exponent = jnp.where(2 * head_ids < H, -5.0 - ids, -math.log2(total_tokens) - (ids - H // 2))
    log_gamma = jnp.log1p(-jnp.exp2(exponent))
    scale = jnp.sqrt(-jnp.expm1(2.0 * log_gamma))
    return (log_gamma, scale)

def span_states(query_three, key_three, value_three, output_grad_three, log_gamma):
    count = query_three.shape[0]
    place = jnp.arange(count, dtype=jnp.float32)[:, None]
    suffix_decay = jnp.exp(log_gamma[None, :] * (count - place))
    prefix_decay = jnp.exp(log_gamma[None, :] * (place + 1.0))
    head_position = lax.Precision.HIGHEST
    forward_sweep = jnp.einsum('ibz,ibm->bzm', key_three.astype(jnp.float32) * suffix_decay[:, :, None], value_three.astype(jnp.float32), precision=head_position)
    backward_sweep = jnp.einsum('stz,stb->tzb', query_three.astype(jnp.float32) * prefix_decay[:, :, None], output_grad_three.astype(jnp.float32), precision=head_position)
    return (forward_sweep, backward_sweep)

def span_grads(query_three, key_three, value_three, output_grad_three, prior_positions, later_positions, log_gamma, scale):
    count = query_three.shape[0]
    head_position = lax.Precision.HIGHEST
    query_flat, key_flat, value_flat, output_grad_flat = (query_three.astype(jnp.float32), key_three.astype(jnp.float32), value_three.astype(jnp.float32), output_grad_three.astype(jnp.float32))
    place = jnp.arange(count, dtype=jnp.float32)
    gap = place[:, None] - place[None, :]
    weight = jnp.where(gap[None] >= 0, scale[:, None, None] * jnp.exp(log_gamma[:, None, None] * jnp.maximum(gap, 0.0)[None]), 0.0)
    local_value_grad = (jnp.einsum('ihv,jhv->hij', output_grad_flat, value_flat) * weight).astype(jnp.bfloat16).astype(jnp.float32)
    local_query_key = (jnp.einsum('ihd,jhd->hij', query_flat, key_flat) * weight).astype(jnp.bfloat16).astype(jnp.float32)
    leading_span = (scale[None, :] * jnp.exp(log_gamma[None, :] * place[:, None]))[:, :, None]
    trailing_span = (scale[None, :] * jnp.exp(log_gamma[None, :] * (count - 1.0 - place[:, None])))[:, :, None]
    query_piece = jnp.einsum('zby,yze->bze', local_value_grad, key_flat) + leading_span * jnp.einsum('eal,gel->gea', prior_positions, output_grad_flat, precision=head_position)
    key_piece = jnp.einsum('lcx,clo->xlo', local_value_grad, query_flat) + trailing_span * jnp.einsum('gta,wga->wgt', later_positions, value_flat, precision=head_position)
    value_piece = jnp.einsum('upb,puk->buk', local_query_key, output_grad_flat) + trailing_span * jnp.einsum('tdx,btd->btx', later_positions, key_flat, precision=head_position)
    return (query_piece, key_piece, value_piece)

def reference(hidden, cotangent, retained, queries, key_rows, value_rows, routes, route_weight, gate_weight, up_weight, down_weight, out_weight):
    target = slot_targets(routes)
    slots = EXPERTS * N_SP * CAP
    upstream = (route_weight[:, :, None] * cotangent[:, None, :].astype(jnp.float32)).astype(jnp.bfloat16).reshape(-1, D)
    inputs = jnp.repeat(hidden, TOP, axis=0)
    up_buffer = jnp.zeros((slots, D), jnp.bfloat16).at[target].set(upstream).reshape(EXPERTS, N_SP * CAP, D)
    in_buffer = jnp.zeros((slots, D), jnp.bfloat16).at[target].set(inputs).reshape(EXPERTS, N_SP * CAP, D)
    gate_grad, up_grad, down_grad, row_grad = lax.map(lambda item: expert_backward(*item), (in_buffer, up_buffer, gate_weight, up_weight, down_weight))
    row_sum = lax.optimization_barrier(jnp.sum(row_grad.astype(jnp.float32), axis=1))
    routed = row_sum.reshape(slots, D)[target].reshape(TOKENS, TOP, D).sum(axis=1)
    layer_grad = (cotangent.astype(jnp.float32) + routed).astype(jnp.bfloat16)
    proj_grad = jnp.dot(layer_grad.T, retained, preferred_element_type=jnp.float32)
    mixed_grad = jnp.dot(layer_grad, out_weight, preferred_element_type=jnp.float32).astype(jnp.bfloat16)
    log_gamma, scale = head_rates(jnp.arange(H, dtype=jnp.int32), TOKENS)
    q5 = queries.reshape(N_SP, TOK_DEV, H, DK)
    k5 = key_rows.reshape(N_SP, TOK_DEV, H, DK)
    v5 = value_rows.reshape(N_SP, TOK_DEV, H, DV)
    do5 = mixed_grad.reshape(N_SP, TOK_DEV, H, DV)
    forward_shard_local, backward_local = lax.map(lambda item: span_states(*item, log_gamma), (q5, k5, v5, do5))
    decay_span = jnp.exp(log_gamma * TOK_DEV)[:, None, None]

    def carry_step(carry, local):
        return (carry * decay_span + local, carry)
    empty = jnp.zeros((H, DK, DV), jnp.float32)
    _, before_all = lax.scan(carry_step, empty, forward_shard_local)
    _, after_all = lax.scan(carry_step, empty, backward_local, reverse=True)
    query_gradient, key_gradient, value_gradient = lax.map(lambda item: span_grads(*item, log_gamma, scale), (q5, k5, v5, do5, before_all, after_all))
    return (gate_grad, up_grad, down_grad, proj_grad, query_gradient.reshape(TOKENS, H * DK), key_gradient.reshape(TOKENS, H * DK), value_gradient.reshape(TOKENS, H * DV))
```

```python
import math

import jax
import jax.numpy as jnp
from jax import lax
from jax.sharding import PartitionSpec as P

H = 4
DK = 256
DV = 512


def carried(part, log_span, axis, reverse):
    count = lax.axis_size(axis)
    held = part
    ahead = jnp.zeros_like(part)
    step = 1
    while step < count:
        pairs = [(i + step, i) if reverse else (i, i + step) for i in range(count - step)]
        got = lax.ppermute(held.astype(jnp.bfloat16), axis, pairs).astype(jnp.float32)
        ahead = ahead + jnp.exp(log_span * (step - 1.0))[:, None, None] * got
        held = held + jnp.exp(log_span * float(step))[:, None, None] * got
        step *= 2
    return ahead


def expert_backward(inputs, upstream, gate_matrix, up_matrix, down_matrix):
    along_rows = (((0,), (0,)), ((), ()))
    along_cols = (((1,), (1,)), ((), ()))
    gate_pre = jnp.dot(inputs, gate_matrix, preferred_element_type=jnp.float32)
    up_pre = jnp.dot(inputs, up_matrix, preferred_element_type=jnp.float32)
    sigma = jax.nn.sigmoid(gate_pre)
    active = gate_pre * sigma
    product = (active * up_pre).astype(jnp.bfloat16)
    down_part = lax.dot_general(product, upstream, along_rows, preferred_element_type=jnp.float32)
    unit_grad = lax.dot_general(
        upstream, down_matrix, along_cols, preferred_element_type=jnp.float32
    )
    gate_term = (unit_grad * up_pre * sigma * (1.0 + gate_pre * (1.0 - sigma))).astype(jnp.bfloat16)
    up_term = (unit_grad * active).astype(jnp.bfloat16)
    gate_part = lax.dot_general(inputs, gate_term, along_rows, preferred_element_type=jnp.float32)
    up_part = lax.dot_general(inputs, up_term, along_rows, preferred_element_type=jnp.float32)
    row_part = lax.dot_general(
        gate_term, gate_matrix, along_cols, preferred_element_type=jnp.float32
    )
    row_part = row_part + lax.dot_general(
        up_term, up_matrix, along_cols, preferred_element_type=jnp.float32
    )
    return (gate_part, up_part, down_part, row_part.astype(jnp.bfloat16))


def head_rates(head_ids, total_tokens):
    ids = head_ids.astype(jnp.float32)
    exponent = jnp.where(2 * head_ids < H, -5.0 - ids, -math.log2(total_tokens) - (ids - H // 2))
    log_gamma = jnp.log1p(-jnp.exp2(exponent))
    scale = jnp.sqrt(-jnp.expm1(2.0 * log_gamma))
    return (log_gamma, scale)


def local(
    hidden,
    cotangent,
    retained,
    queries,
    key_rows,
    value_rows,
    routes,
    route_weight,
    gate_weight,
    up_weight,
    down_weight,
    out_weight,
):
    sp_count = lax.axis_size("sp")
    tp_count = lax.axis_size("tp")
    tok_local = hidden.shape[0]
    width = hidden.shape[1]
    top_count = routes.shape[1]
    experts_all = gate_weight.shape[0] * sp_count
    capacity = 3 * tok_local * top_count // (2 * experts_all)
    ids = jnp.arange(experts_all, dtype=jnp.int32)[:, None]
    named = [routes[:, r][None, :] == ids for r in range(top_count)]
    member = sum(m.astype(jnp.float32) for m in named)
    slot_weight = sum(jnp.where(m, route_weight[:, r][None, :], 0.0) for r, m in enumerate(named))
    order = jnp.arange(tok_local, dtype=jnp.int32)
    earlier = (order[:, None] < order[None, :]).astype(jnp.bfloat16)
    rank = jnp.dot(member.astype(jnp.bfloat16), earlier, preferred_element_type=jnp.float32)
    rank = jnp.where(member > 0.0, rank, -1.0).astype(jnp.int32)
    hit = rank[:, None, :] == jnp.arange(capacity, dtype=jnp.int32)[None, :, None]
    place_rows = hit.astype(jnp.bfloat16).reshape(experts_all * capacity, tok_local)
    row_weight = jnp.sum(jnp.where(hit, slot_weight[:, None, :], 0.0), axis=2).reshape(-1, 1)
    col_width = width // tp_count
    col_start = lax.axis_index("tp") * col_width
    hid_cols = lax.dynamic_slice_in_dim(hidden, col_start, col_width, 1)
    cot_cols = lax.dynamic_slice_in_dim(cotangent, col_start, col_width, 1)

    def to_experts(rows):
        rows = rows.astype(jnp.bfloat16).reshape(experts_all, capacity, col_width)
        return lax.all_to_all(rows, "sp", split_axis=0, concat_axis=1, tiled=True)

    in_cols = to_experts(jnp.dot(place_rows, hid_cols, preferred_element_type=jnp.float32))
    up_cols = to_experts(
        row_weight * jnp.dot(place_rows, cot_cols, preferred_element_type=jnp.float32)
    )
    got_in = lax.all_gather(in_cols, "tp", axis=2, tiled=True)
    got_up = lax.all_gather(up_cols, "tp", axis=2, tiled=True)
    gate_grad, up_grad, down_grad, row_part = jax.vmap(expert_backward)(
        got_in, got_up, gate_weight, up_weight, down_weight
    )
    row_grad = lax.psum_scatter(row_part, "tp", scatter_dimension=2, tiled=True)
    returned = lax.all_to_all(row_grad, "sp", split_axis=1, concat_axis=0, tiled=True)
    routed = lax.dot_general(
        place_rows,
        returned.reshape(-1, col_width),
        (((0,), (0,)), ((), ())),
        preferred_element_type=jnp.float32,
    )
    layer_cols = (cot_cols.astype(jnp.float32) + routed).astype(jnp.bfloat16)
    layer_grad = lax.all_gather(layer_cols, "tp", axis=1, tiled=True)
    proj_grad = lax.psum_scatter(
        lax.dot_general(
            layer_grad, retained, (((0,), (0,)), ((), ())), preferred_element_type=jnp.float32
        ).astype(jnp.bfloat16),
        "sp",
        scatter_dimension=0,
        tiled=True,
    ).astype(jnp.float32)
    mixed_grad = jnp.dot(layer_grad, out_weight, preferred_element_type=jnp.float32).astype(
        jnp.bfloat16
    )
    heads_local = queries.shape[1] // DK
    head_ids = lax.axis_index("tp") * heads_local + jnp.arange(heads_local, dtype=jnp.int32)
    log_gamma, scale = head_rates(head_ids, tok_local * sp_count)
    query_three = queries.reshape(tok_local, heads_local, DK)
    key_three = key_rows.reshape(tok_local, heads_local, DK)
    value_three = value_rows.reshape(tok_local, heads_local, DV)
    output_grad_three = mixed_grad.reshape(tok_local, heads_local, DV)
    place = jnp.arange(tok_local, dtype=jnp.float32)
    suffix_decay = jnp.exp(log_gamma[None, :] * (tok_local - place[:, None]))
    prefix_decay = jnp.exp(log_gamma[None, :] * (place[:, None] + 1.0))
    forward_shard_local = jnp.einsum(
        "ibz,ibm->bzm",
        (key_three * suffix_decay[:, :, None]).astype(jnp.bfloat16),
        value_three,
        preferred_element_type=jnp.float32,
    )
    backward_local = jnp.einsum(
        "stz,stb->tzb",
        (query_three * prefix_decay[:, :, None]).astype(jnp.bfloat16),
        output_grad_three,
        preferred_element_type=jnp.float32,
    )
    log_span = log_gamma * tok_local
    prior_positions = carried(forward_shard_local, log_span, "sp", False).astype(jnp.bfloat16)
    later_positions = carried(backward_local, log_span, "sp", True).astype(jnp.bfloat16)
    gap = place[:, None] - place[None, :]
    weight = jnp.where(
        gap[None] >= 0,
        scale[:, None, None] * jnp.exp(log_gamma[:, None, None] * jnp.maximum(gap, 0.0)[None]),
        0.0,
    )
    local_value_grad = (
        jnp.einsum(
            "ihv,jhv->hij", output_grad_three, value_three, preferred_element_type=jnp.float32
        )
        * weight
    ).astype(jnp.bfloat16)
    local_query_key = (
        jnp.einsum("ihd,jhd->hij", query_three, key_three, preferred_element_type=jnp.float32)
        * weight
    ).astype(jnp.bfloat16)
    leading_span = (scale[None, :] * jnp.exp(log_gamma[None, :] * place[:, None]))[:, :, None]
    trailing_span = (
        scale[None, :] * jnp.exp(log_gamma[None, :] * (tok_local - 1.0 - place[:, None]))
    )[:, :, None]
    query_gradient = jnp.einsum(
        "zby,yze->bze", local_value_grad, key_three, preferred_element_type=jnp.float32
    )
    query_gradient = query_gradient + leading_span * jnp.einsum(
        "eal,gel->gea", prior_positions, output_grad_three, preferred_element_type=jnp.float32
    )
    key_gradient = jnp.einsum(
        "lcx,clo->xlo", local_value_grad, query_three, preferred_element_type=jnp.float32
    )
    key_gradient = key_gradient + trailing_span * jnp.einsum(
        "gta,wga->wgt", later_positions, value_three, preferred_element_type=jnp.float32
    )
    value_gradient = jnp.einsum(
        "upb,puk->buk", local_query_key, output_grad_three, preferred_element_type=jnp.float32
    )
    value_gradient = value_gradient + trailing_span * jnp.einsum(
        "tdx,btd->btx", later_positions, key_three, preferred_element_type=jnp.float32
    )
    return (
        gate_grad,
        up_grad,
        down_grad,
        proj_grad,
        query_gradient.reshape(tok_local, heads_local * DK),
        key_gradient.reshape(tok_local, heads_local * DK),
        value_gradient.reshape(tok_local, heads_local * DV),
    )


def solution(mesh):
    return jax.shard_map(
        local,
        mesh=mesh,
        in_specs=(
            P("sp", None),
            P("sp", None),
            P("sp", "tp"),
            P("sp", "tp"),
            P("sp", "tp"),
            P("sp", "tp"),
            P("sp", None),
            P("sp", None),
            P("sp", None, "tp"),
            P("sp", None, "tp"),
            P("sp", "tp", None),
            P(None, "tp"),
        ),
        out_specs=(
            P("sp", None, "tp"),
            P("sp", None, "tp"),
            P("sp", "tp", None),
            P("sp", "tp"),
            P("sp", "tp"),
            P("sp", "tp"),
            P("sp", "tp"),
        ),
        check_vma=False,
    )
```

```python
import math

import jax
import jax.numpy as jnp
from jax import lax
from jax.sharding import PartitionSpec as P

H = 4
DK = 256
DV = 512


def carried(part, log_span, axis, reverse):
    count = lax.axis_size(axis)
    held = part
    ahead = jnp.zeros_like(part)
    step = 1
    while step < count:
        pairs = [(i + step, i) if reverse else (i, i + step) for i in range(count - step)]
        got = lax.ppermute(held.astype(jnp.bfloat16), axis, pairs).astype(jnp.float32)
        ahead = ahead + jnp.exp(log_span * (step - 1.0))[:, None, None] * got
        held = held + jnp.exp(log_span * float(step))[:, None, None] * got
        step *= 2
    return ahead


def scattered_sum(part, axis):
    count = lax.axis_size(axis)
    me = lax.axis_index(axis)
    if count & (count - 1):
        return lax.psum_scatter(part, axis, scatter_dimension=2, tiled=True)
    wide = part.shape[2] // count
    pieces = {
        k: lax.dynamic_slice_in_dim(part, jnp.bitwise_xor(me, k) * wide, wide, 2)
        for k in range(count)
    }
    bit = 1
    while bit < count:
        pairs = [(i, i ^ bit) for i in range(count)]
        for k in sorted(k for k in pieces if k & bit):
            got = lax.ppermute(pieces.pop(k), axis, pairs)
            kept = pieces[k ^ bit].astype(jnp.float32)
            pieces[k ^ bit] = (kept + got.astype(jnp.float32)).astype(jnp.bfloat16)
        bit *= 2
    return pieces[0]


def expert_backward(inputs, upstream, gate_matrix, up_matrix, down_matrix):
    along_rows = (((0,), (0,)), ((), ()))
    along_cols = (((1,), (1,)), ((), ()))
    gate_pre = jnp.dot(inputs, gate_matrix, preferred_element_type=jnp.float32)
    up_pre = jnp.dot(inputs, up_matrix, preferred_element_type=jnp.float32)
    sigma = jax.nn.sigmoid(gate_pre)
    active = gate_pre * sigma
    product = (active * up_pre).astype(jnp.bfloat16)
    down_part = lax.dot_general(product, upstream, along_rows, preferred_element_type=jnp.float32)
    unit_grad = lax.dot_general(
        upstream, down_matrix, along_cols, preferred_element_type=jnp.float32
    )
    gate_term = (unit_grad * up_pre * sigma * (1.0 + gate_pre * (1.0 - sigma))).astype(jnp.bfloat16)
    up_term = (unit_grad * active).astype(jnp.bfloat16)
    gate_part = lax.dot_general(inputs, gate_term, along_rows, preferred_element_type=jnp.float32)
    up_part = lax.dot_general(inputs, up_term, along_rows, preferred_element_type=jnp.float32)
    row_part = lax.dot_general(
        gate_term, gate_matrix, along_cols, preferred_element_type=jnp.float32
    )
    row_part = row_part + lax.dot_general(
        up_term, up_matrix, along_cols, preferred_element_type=jnp.float32
    )
    return (gate_part, up_part, down_part, row_part.astype(jnp.bfloat16))


def head_rates(head_ids, total_tokens):
    ids = head_ids.astype(jnp.float32)
    exponent = jnp.where(2 * head_ids < H, -5.0 - ids, -math.log2(total_tokens) - (ids - H // 2))
    log_gamma = jnp.log1p(-jnp.exp2(exponent))
    scale = jnp.sqrt(-jnp.expm1(2.0 * log_gamma))
    return (log_gamma, scale)


def local(
    hidden,
    cotangent,
    retained,
    queries,
    key_rows,
    value_rows,
    routes,
    route_weight,
    gate_weight,
    up_weight,
    down_weight,
    out_weight,
):
    sp_count = lax.axis_size("sp")
    tp_count = lax.axis_size("tp")
    tok_local = hidden.shape[0]
    width = hidden.shape[1]
    top_count = routes.shape[1]
    experts_all = gate_weight.shape[0] * sp_count
    capacity = 3 * tok_local * top_count // (2 * experts_all)
    ids = jnp.arange(experts_all, dtype=jnp.int32)[:, None]
    named = [routes[:, r][None, :] == ids for r in range(top_count)]
    member = sum(m.astype(jnp.float32) for m in named)
    slot_weight = sum(jnp.where(m, route_weight[:, r][None, :], 0.0) for r, m in enumerate(named))
    order = jnp.arange(tok_local, dtype=jnp.int32)
    earlier = (order[:, None] < order[None, :]).astype(jnp.bfloat16)
    rank = jnp.dot(member.astype(jnp.bfloat16), earlier, preferred_element_type=jnp.float32)
    rank = jnp.where(member > 0.0, rank, -1.0).astype(jnp.int32)
    hit = rank[:, None, :] == jnp.arange(capacity, dtype=jnp.int32)[None, :, None]
    place_rows = hit.astype(jnp.bfloat16).reshape(experts_all * capacity, tok_local)
    row_weight = jnp.sum(jnp.where(hit, slot_weight[:, None, :], 0.0), axis=2).reshape(-1, 1)
    col_width = width // tp_count
    col_start = lax.axis_index("tp") * col_width
    hid_cols = lax.dynamic_slice_in_dim(hidden, col_start, col_width, 1)
    cot_cols = lax.dynamic_slice_in_dim(cotangent, col_start, col_width, 1)

    def to_experts(rows):
        rows = rows.astype(jnp.bfloat16).reshape(experts_all, capacity, col_width)
        return lax.all_to_all(rows, "sp", split_axis=0, concat_axis=1, tiled=True)

    in_cols = to_experts(jnp.dot(place_rows, hid_cols, preferred_element_type=jnp.float32))
    in_cols, cot_cols = lax.optimization_barrier((in_cols, cot_cols))
    up_cols = to_experts(
        row_weight * jnp.dot(place_rows, cot_cols, preferred_element_type=jnp.float32)
    )
    heads_local = queries.shape[1] // DK
    head_ids = lax.axis_index("tp") * heads_local + jnp.arange(heads_local, dtype=jnp.int32)
    log_gamma, scale = head_rates(head_ids, tok_local * sp_count)
    key_rows, value_rows, up_cols = lax.optimization_barrier((key_rows, value_rows, up_cols))
    query_three = queries.reshape(tok_local, heads_local, DK)
    key_three = key_rows.reshape(tok_local, heads_local, DK)
    value_three = value_rows.reshape(tok_local, heads_local, DV)
    place = jnp.arange(tok_local, dtype=jnp.float32)
    suffix_decay = jnp.exp(log_gamma[None, :] * (tok_local - place[:, None]))
    prefix_decay = jnp.exp(log_gamma[None, :] * (place[:, None] + 1.0))
    forward_shard_local = jnp.einsum(
        "ibz,ibm->bzm",
        (key_three * suffix_decay[:, :, None]).astype(jnp.bfloat16),
        value_three,
        preferred_element_type=jnp.float32,
    )
    log_span = log_gamma * tok_local
    prior_positions = carried(forward_shard_local, log_span, "sp", False).astype(jnp.bfloat16)
    got_in = lax.all_gather(in_cols, "tp", axis=2, tiled=True)
    got_up = lax.all_gather(up_cols, "tp", axis=2, tiled=True)
    retained, got_up = lax.optimization_barrier((retained, got_up))
    retained_all = lax.all_gather(retained, "sp", axis=0, tiled=True)
    gate_grad, up_grad, down_grad, row_part = jax.vmap(expert_backward)(
        got_in, got_up, gate_weight, up_weight, down_weight
    )
    row_part, prior_positions = lax.optimization_barrier((row_part, prior_positions))
    row_grad = scattered_sum(row_part, "tp")
    row_grad = row_grad.reshape(-1, sp_count, capacity, col_width).swapaxes(0, 1)
    returned = lax.all_to_all(row_grad, "sp", split_axis=0, concat_axis=0, tiled=True)
    returned, retained_all = lax.optimization_barrier((returned, retained_all))
    routed = lax.dot_general(
        place_rows,
        returned.reshape(-1, col_width),
        (((0,), (0,)), ((), ())),
        preferred_element_type=jnp.float32,
    )
    layer_cols = (cot_cols.astype(jnp.float32) + routed).astype(jnp.bfloat16)
    layer_grad = lax.all_gather(layer_cols, "tp", axis=1, tiled=True)
    mixed_grad = jnp.dot(layer_grad, out_weight, preferred_element_type=jnp.float32).astype(
        jnp.bfloat16
    )
    share = tok_local // tp_count
    share_rows = lax.dynamic_slice_in_dim(layer_grad, lax.axis_index("tp") * share, share, 0)
    share_rows = share_rows.reshape(share, sp_count, -1).swapaxes(0, 1)
    block_rows = lax.all_to_all(share_rows, "sp", split_axis=0, concat_axis=0, tiled=True)
    block_all = lax.all_gather(block_rows, "tp", axis=1, tiled=True)
    proj_grad = lax.dot_general(
        block_all.reshape(sp_count * tok_local, -1),
        retained_all,
        (((0,), (0,)), ((), ())),
        preferred_element_type=jnp.float32,
    )
    output_grad_three = mixed_grad.reshape(tok_local, heads_local, DV)
    backward_local = jnp.einsum(
        "stz,stb->tzb",
        (query_three * prefix_decay[:, :, None]).astype(jnp.bfloat16),
        output_grad_three,
        preferred_element_type=jnp.float32,
    )
    later_positions = carried(backward_local, log_span, "sp", True).astype(jnp.bfloat16)
    gap = place[:, None] - place[None, :]
    weight = jnp.where(
        gap[None] >= 0,
        scale[:, None, None] * jnp.exp(log_gamma[:, None, None] * jnp.maximum(gap, 0.0)[None]),
        0.0,
    )
    local_value_grad = (
        jnp.einsum(
            "ihv,jhv->hij", output_grad_three, value_three, preferred_element_type=jnp.float32
        )
        * weight
    ).astype(jnp.bfloat16)
    local_query_key = (
        jnp.einsum("ihd,jhd->hij", query_three, key_three, preferred_element_type=jnp.float32)
        * weight
    ).astype(jnp.bfloat16)
    leading_span = (scale[None, :] * jnp.exp(log_gamma[None, :] * place[:, None]))[:, :, None]
    trailing_span = (
        scale[None, :] * jnp.exp(log_gamma[None, :] * (tok_local - 1.0 - place[:, None]))
    )[:, :, None]
    query_gradient = jnp.einsum(
        "zby,yze->bze", local_value_grad, key_three, preferred_element_type=jnp.float32
    )
    query_gradient = query_gradient + leading_span * jnp.einsum(
        "eal,gel->gea", prior_positions, output_grad_three, preferred_element_type=jnp.float32
    )
    key_gradient = jnp.einsum(
        "lcx,clo->xlo", local_value_grad, query_three, preferred_element_type=jnp.float32
    )
    key_gradient = key_gradient + trailing_span * jnp.einsum(
        "gta,wga->wgt", later_positions, value_three, preferred_element_type=jnp.float32
    )
    value_gradient = jnp.einsum(
        "upb,puk->buk", local_query_key, output_grad_three, preferred_element_type=jnp.float32
    )
    value_gradient = value_gradient + trailing_span * jnp.einsum(
        "tdx,btd->btx", later_positions, key_three, preferred_element_type=jnp.float32
    )
    return (
        gate_grad,
        up_grad,
        down_grad,
        proj_grad,
        query_gradient.reshape(tok_local, heads_local * DK),
        key_gradient.reshape(tok_local, heads_local * DK),
        value_gradient.reshape(tok_local, heads_local * DV),
    )


def solution(mesh):
    return jax.shard_map(
        local,
        mesh=mesh,
        in_specs=(
            P("sp", None),
            P("sp", None),
            P("sp", "tp"),
            P("sp", "tp"),
            P("sp", "tp"),
            P("sp", "tp"),
            P("sp", None),
            P("sp", None),
            P("sp", None, "tp"),
            P("sp", None, "tp"),
            P("sp", "tp", None),
            P(None, "tp"),
        ),
        out_specs=(
            P("sp", None, "tp"),
            P("sp", None, "tp"),
            P("sp", "tp", None),
            P("sp", "tp"),
            P("sp", "tp"),
            P("sp", "tp"),
            P("sp", "tp"),
        ),
        check_vma=False,
    )
```
